32 devices in a mesh: sp: 8 (over z, core), tp: 4 (over y, x).
Axes of the slice: x: 2, y: 2, z: 4, core: 2. Of those that a mesh axis runs over, the one named last changes fastest.
Arguments:
- moe_input: bfloat16 [2560, 2048], P('sp', 'tp'), may hold values from -6 to 6
- out_cotangent: bfloat16 [2560, 2048], P('sp', 'tp'), may hold values from -0.59765625 to 0.59765625
- routes: int32 [2560, 2], P('sp'), may hold values from 0 to 7, all different within a row; in each aligned block of 320 rows (0 to 319, 320 to 639, ...) at most 120 rows name the same one
- route_weight: float32 [2560, 2], P('sp'), may hold values from 0.1 to 0.9
- gate_weight: bfloat16 [8, 1024, 2048], P('sp', 'tp'), may hold values from -0.125 to 0.125
- up_weight: bfloat16 [8, 1024, 2048], P('sp', 'tp'), may hold values from -0.125 to 0.125
- down_weight: bfloat16 [8, 1024, 2048], P('sp', 'tp'), may hold values from -0.1875 to 0.1875
- glu_value: bfloat16 [2560, 1024], P('sp', 'tp'), may hold values from -6 to 6
- glu_gate: bfloat16 [2560, 1024], P('sp', 'tp'), may hold values from -8 to 8
- conv_result: bfloat16 [2560, 1024], P('sp', 'tp'), may hold values from -12 to 12
- conv_taps: float32 [31, 1024], P(None, 'tp'), may hold values from -1 to 1
- norm_gain: float32 [1024], P('tp'), may hold values from 0.1 to 1.9
- proj_weight: bfloat16 [1024, 2048], P('tp'), may hold values from -0.1875 to 0.1875
Outputs:
- grad_gate: float32 [8, 1024, 2048], P('sp', 'tp')
- grad_up: float32 [8, 1024, 2048], P('sp', 'tp')
- grad_down: float32 [8, 1024, 2048], P('sp', 'tp')
- grad_proj: float32 [2048, 1024], P('sp', 'tp')
- grad_value: bfloat16 [2560, 1024], P('sp', 'tp')
- grad_glu_gate: bfloat16 [2560, 1024], P('sp', 'tp')
The draws below stay inside these ranges and needn't reach their ends.
Inputs may be any that keep to these rules, and one draw needn't show every extreme that they name: `routes`: each row names two different experts. In the aligned blocks of 320 rows (the rows of one index of sp) no expert is named by more than 120 rows, and that bound is reached.
All inputs are finite; a program needn't handle non-finite values.
Results may differ from the reference program's by a relative error of at most 0.025.
Values may be sent and summed in bfloat16 or wider, within the bound.
A program may use at most 64 MiB of HBM per device.

```python
import math
import jax
import jax.numpy as jnp
import numpy as np
from jax import lax

D = 2048
C = 1024
F = 1024
K = 31
TOK_DEV = 320
TOKENS = 2560
EXPERTS = 8
CAP = 120
SLOTS = 960
FT = 256
N_SP = 8
N_TP = 4


def draw_conv_result(key, part):
    first, second, third = jax.random.split(key, 3)
    position = jnp.arange(C, dtype=jnp.float32) / C
    chan_scale = (0.5 + 2.5 * position) * jax.random.uniform(first, (C,), jnp.float32, 0.7, 1.4)
    offset = jax.random.uniform(second, (C,), jnp.float32, -1.0, 1.0)
    base = jax.random.normal(third, (TOKENS, C), jnp.float32)
    values = base * chan_scale[None, :] + offset[None, :]
    return jnp.clip(values, -12.0, 12.0).astype(jnp.bfloat16)


def raised(values, rng, source, target, parts, factor):
    def block_of(dim):
        return (jnp.arange(values.shape[dim]) // (values.shape[dim] // parts)).reshape((-1,) + (1,) * (values.ndim - 1 - dim))

    one_side = jax.random.permutation(rng, parts)[block_of(target)]
    second = (block_of(target) + parts // 2) % parts
    return jnp.where((block_of(source) == one_side) | (block_of(source) == second), factor * values, values)


def level_of(key, dims, cuts, least, high):
    loudness = 1.0
    for dim, blocks in cuts:
        steps = jax.random.uniform(jax.random.fold_in(jax.random.fold_in(key, 6), dim), (blocks,), jnp.float32, least / len(cuts), high / len(cuts))
        loudness = loudness * jnp.repeat(jnp.exp(steps), dims[dim] // blocks).reshape((-1,) + (1,) * (len(dims) - 1 - dim))
    return loudness


def assign_block(stream_key, own, number, rows, number_of, top, reach, skew):
    ranking = jax.random.permutation(stream_key, number_of)
    crowded, common = load_shares(number_of, rows * top, reach, skew, True), load_shares(number_of, rows * top, reach, skew, False)
    places = jnp.arange(number_of)

    def named(sizes, rotation):
        used = int((sizes > 0).sum())
        fixed = max(1, used // 4)
        passed = fixed + (places - fixed + rotation * (used - fixed)) % max(1, number_of - fixed)
        return jnp.zeros((number_of,), jnp.int32).at[ranking[jnp.where(places < fixed, places, passed)]].set(jnp.asarray(sizes, jnp.int32))

    sizes = jnp.where(number % 4 == 0, named(crowded, number // 4), named(common, number - number // 4 - 1))
    mixed = jax.random.permutation(jax.random.fold_in(own, 3), number_of)
    source_of, sink = mixed[0:number_of // 2 * 2:2], mixed[1:number_of // 2 * 2:2]
    room = jnp.minimum(sizes[source_of] - 1, reach - sizes[sink]) // 2
    room = jnp.where((source_of == ranking[0]) | (sink == ranking[0]) | (sizes[sink] == 0), 0, jnp.maximum(room, 0))
    passed = jax.random.randint(jax.random.fold_in(own, 4), (number_of // 2,), 0, 1 << 20) % (room + 1)
    sizes = sizes.at[source_of].add(-passed).at[sink].add(passed)
    labels = jnp.searchsorted(jnp.cumsum(sizes), jnp.arange(rows * top), side="right").astype(jnp.int32)
    grid = labels.reshape(top, rows).T
    grid = grid[jax.random.permutation(jax.random.fold_in(own, 1), rows)]
    rotation = jax.random.randint(jax.random.fold_in(own, 2), (rows, 1), 0, top)
    return jnp.take_along_axis(grid, (jnp.arange(top)[None, :] + rotation) % top, axis=1)


def load_shares(count, total, most, slope, full):
    weights = [(1 << 20) // math.isqrt(standing ** slope) + 1 for standing in range(1, count + 1)]
    largest = most if full else min(most, max(-(-total // count), total * weights[0] // sum(weights)))
    least = 1 if total - largest >= count - 1 else 0
    counts, surplus = [largest] + [least] * (count - 1), total - largest - least * (count - 1)
    while surplus > 0:
        free = [i for i in range(1, count) if counts[i] < largest] or [i for i in range(1, count) if counts[i] < most]
        whole, remaining = sum([weights[i] for i in free]), surplus
        for i in free:
            extra = min(most - counts[i], max(1, remaining * weights[i] // whole), surplus)
            counts[i] = counts[i] + extra
            surplus = surplus - extra
    return np.array(counts)


def noise(key, shape, deviation, reach, shards=(), kind=jnp.bfloat16):
    level = level_of(key, shape, shards, -0.22, 0.18) if shards else 1.0
    values = jax.random.normal(key, shape, jnp.float32) * deviation * level
    return jnp.minimum(jnp.maximum(values, -reach), reach).astype(kind)


def heavy_noise(key, shape, width, bound, cuts, heavy, kind=jnp.bfloat16):
    values = width * jax.random.normal(key, shape, jnp.float32)
    if cuts:
        values = values * level_of(key, shape, cuts, -0.22, 0.18)
    return jnp.clip(raised(values, jax.random.fold_in(key, 3), *heavy), -bound, bound).astype(kind)


def setup_inputs(seed: int = 0) -> dict:
    arg_keys = jax.random.split(jax.random.key(seed), 14)
    moe_input = noise(arg_keys[0], (TOKENS, D), 1.0, 6.0, ((0, 8), (1, 4)))
    out_cotangent = heavy_noise(arg_keys[1], (TOKENS, D), 0.1, 0.59765625, ((0, 8), (1, 4)), (0, 1, 8, 2.0))
    routes_keys = jax.random.split(jax.random.fold_in(arg_keys[2], 1), TOKENS // TOK_DEV)
    routes_turns = jax.random.permutation(jax.random.fold_in(arg_keys[2], 3), TOKENS // TOK_DEV)
    routes = jax.vmap(lambda own, number: assign_block(jax.random.fold_in(arg_keys[2], 2), own, number, TOK_DEV, EXPERTS, 2, CAP, 2))(routes_keys, routes_turns).reshape((TOKENS, 2))
    route_weight = jnp.clip(0.1 + 0.79999997 * jax.random.uniform(arg_keys[3], (TOKENS, 2), jnp.float32) ** level_of(arg_keys[3], (TOKENS, 2), ((0, 8),), -0.2, 0.2), 0.1, 0.9)
    gate_weight = noise(arg_keys[4], (EXPERTS, F, D), D ** -0.5, 0.125, ((0, 8), (1, 4)))
    up_weight = noise(arg_keys[5], (EXPERTS, F, D), D ** -0.5, 0.125, ((0, 8), (1, 4)))
    down_weight = noise(arg_keys[6], (EXPERTS, F, D), F ** -0.5, 0.1875, ((0, 8), (1, 4)))
    glu_value = noise(arg_keys[7], (TOKENS, C), 1.0, 6.0, ((0, 8), (1, 4)))
    glu_gate = noise(arg_keys[8], (TOKENS, C), 1.5, 8.0, ((0, 8), (1, 4)))
    conv_result = draw_conv_result(jax.random.fold_in(arg_keys[13], 71), 0)
    conv_taps = noise(arg_keys[10], (K, C), K ** -0.5, 1.0, ((1, 4),), jnp.float32)
    norm_gain = jnp.clip(1.0 + 0.18 * jax.random.normal(arg_keys[11], (C,), jnp.float32), 0.1, 1.9)
    proj_weight = noise(arg_keys[12], (C, D), C ** -0.5, 0.1875, ((0, 4),))
    return {"moe_input": moe_input, "out_cotangent": out_cotangent, "routes": routes, "route_weight": route_weight, "gate_weight": gate_weight, "up_weight": up_weight, "down_weight": down_weight, "glu_value": glu_value, "glu_gate": glu_gate, "conv_result": conv_result, "conv_taps": conv_taps, "norm_gain": norm_gain, "proj_weight": proj_weight}


NORM_EPS = 0.25

def pair_places(routes):
    blocks = routes.reshape(N_SP, TOK_DEV * 2).astype(jnp.int32)
    onehot = (blocks[:, :, None] == jnp.arange(EXPERTS, dtype=jnp.int32)[None, None, :]).astype(jnp.int32)
    earlier = jnp.cumsum(onehot, axis=1) - onehot
    slot_rank = lax.optimization_barrier(jnp.sum(earlier * onehot, axis=2))
    source = jnp.arange(N_SP, dtype=jnp.int32)[:, None]
    places = (source * CAP + slot_rank).reshape(-1).astype(jnp.int32)
    return (routes.reshape(-1).astype(jnp.int32), places)

def contract_rows(left, right):
    return lax.dot_general(left, right, (((0,), (0,)), ((), ())), preferred_element_type=jnp.float32)

def contract_cols(left, right):
    return lax.dot_general(left, right, (((1,), (1,)), ((), ())), preferred_element_type=jnp.float32)

def expert_backward(packed):
    token_rows, cot_rows, gate_matrix, up_matrix, down_matrix = packed
    gate_pre = contract_cols(token_rows, gate_matrix)
    up_pre = contract_cols(token_rows, up_matrix)
    gate_sigmoid = jax.nn.sigmoid(gate_pre)
    activation = gate_pre * gate_sigmoid
    hidden = (activation * up_pre).astype(jnp.bfloat16)
    grad_down = contract_rows(hidden, cot_rows)
    hidden_cot = contract_cols(cot_rows, down_matrix)
    up_cot = (hidden_cot * activation).astype(jnp.bfloat16)
    gate_cot = (hidden_cot * up_pre * gate_sigmoid * (1.0 + gate_pre * (1.0 - gate_sigmoid))).astype(jnp.bfloat16)
    grad_gate = contract_rows(gate_cot, token_rows)
    grad_up = contract_rows(up_cot, token_rows)
    gate_blocks = gate_cot.astype(jnp.float32).reshape(SLOTS, N_TP, FT)
    up_blocks = up_cot.astype(jnp.float32).reshape(SLOTS, N_TP, FT)
    gate_wblocks = gate_matrix.astype(jnp.float32).reshape(N_TP, FT, D)
    up_wblocks = up_matrix.astype(jnp.float32).reshape(N_TP, FT, D)
    partial_value = jnp.einsum('rtf,tfd->trd', gate_blocks, gate_wblocks) + jnp.einsum('rtf,tfd->trd', up_blocks, up_wblocks)
    rounded = lax.optimization_barrier(partial_value.astype(jnp.bfloat16))
    returned = lax.optimization_barrier(jnp.sum(rounded.astype(jnp.float32), axis=0)).astype(jnp.bfloat16)
    return (grad_gate, grad_up, grad_down, returned)

def reference(moe_input, out_cotangent, routes, route_weight, gate_weight, up_weight, down_weight, glu_value, glu_gate, conv_result, conv_taps, norm_gain, proj_weight):
    expert_ids, places = pair_places(routes)
    pair_rows = jnp.repeat(moe_input, 2, axis=0)
    scaled = (route_weight.reshape(-1, 1) * jnp.repeat(out_cotangent, 2, axis=0).astype(jnp.float32)).astype(jnp.bfloat16)
    expert_rows = jnp.zeros((EXPERTS, SLOTS, D), jnp.bfloat16).at[expert_ids, places].set(pair_rows)
    expert_cot = jnp.zeros((EXPERTS, SLOTS, D), jnp.bfloat16).at[expert_ids, places].set(scaled)
    grad_gate, grad_up, grad_down, returned = lax.map(expert_backward, (expert_rows, expert_cot, gate_weight, up_weight, down_weight))
    picked = returned[expert_ids, places].astype(jnp.float32)
    moe_grad = lax.optimization_barrier(jnp.sum(picked.reshape(TOKENS, 2, D), axis=1))
    total_cot = (out_cotangent.astype(jnp.float32) + moe_grad).astype(jnp.bfloat16)
    conv_values = conv_result.astype(jnp.float32)
    row_mean = lax.optimization_barrier(jnp.mean(conv_values, axis=1, keepdims=True))
    centered = conv_values - row_mean
    inv_scale = lax.rsqrt(lax.optimization_barrier(jnp.mean(centered * centered, axis=1, keepdims=True)) + NORM_EPS)
    normed = centered * inv_scale
    linear = normed * norm_gain[None, :]
    lin_sigmoid = jax.nn.sigmoid(linear)
    act_out = (linear * lin_sigmoid).astype(jnp.bfloat16)
    grad_proj = contract_rows(total_cot, act_out)
    act_cot = contract_cols(total_cot, proj_weight)
    norm_cot = act_cot * lin_sigmoid * (1.0 + linear * (1.0 - lin_sigmoid)) * norm_gain[None, :]
    conv_cot = inv_scale * (norm_cot - lax.optimization_barrier(jnp.mean(norm_cot, axis=1, keepdims=True)) - normed * lax.optimization_barrier(jnp.mean(norm_cot * normed, axis=1, keepdims=True)))
    padded = jnp.pad(conv_cot, ((0, K - 1), (0, 0)))
    glu_cot = lax.conv_general_dilated(padded[None], jnp.flip(conv_taps, 0)[:, None, :], (1,), 'VALID', dimension_numbers=('NWC', 'WIO', 'NWC'), feature_group_count=C, precision=lax.Precision.HIGHEST)[0]
    gate_sigmoid = jax.nn.sigmoid(glu_gate.astype(jnp.float32))
    grad_value = (glu_cot * gate_sigmoid).astype(jnp.bfloat16)
    grad_glu_gate = (glu_cot * glu_value.astype(jnp.float32) * gate_sigmoid * (1.0 - gate_sigmoid)).astype(jnp.bfloat16)
    return (grad_gate, grad_up, grad_down, grad_proj, grad_value, grad_glu_gate)
```

```python
import functools

import jax
import jax.numpy as jnp
from jax import lax
from jax.experimental import pallas as pl
from jax.experimental.pallas import tpu as pltpu
from jax.sharding import PartitionSpec as P

C = 1024


NORM_EPS = 0.25


MESH = pl.DeviceIdType.MESH


def from_behind(value, axis, steps):
    count = lax.axis_size(axis)
    leading, last = (max(0, -steps), min(count, count - steps))
    return lax.ppermute(value, axis, [(source, source + steps) for source in range(leading, last)])


def pair_places(route_ids, experts, capacity):
    flat_ids = route_ids.reshape(-1)
    onehot = (flat_ids[:, None] == jnp.arange(experts, dtype=jnp.int32)[None, :]).astype(jnp.int32)
    earlier = jnp.cumsum(onehot, axis=0) - onehot
    slot_rank = jnp.sum(earlier * onehot, axis=1)
    return flat_ids * capacity + slot_rank


def place_rows(values, target, experts, capacity):
    empty_rows = jnp.zeros((experts * capacity, values.shape[1]), values.dtype)
    return empty_rows.at[target].set(values).reshape(experts, capacity, values.shape[1])


def flip(index, mask):
    result, bit = index, 1
    while bit <= mask:
        if mask & bit:
            result = result + bit * (1 - 2 * ((index // bit) % 2))
        bit *= 2
    return result


def greet(sp, tp, n_sp, n_tp):
    barrier = pltpu.get_barrier_semaphore()
    for mask in range(1, n_sp):
        pl.semaphore_signal(barrier, inc=1, device_id=(flip(sp, mask), tp), device_id_type=MESH)
    for mask in range(1, n_tp):
        pl.semaphore_signal(barrier, inc=1, device_id=(sp, flip(tp, mask)), device_id_type=MESH)
    pl.semaphore_wait(barrier, n_sp + n_tp - 2)


def columns(index, width):
    return pl.ds(pl.multiple_of(index * width, width), width)


def dispatch_kernel(
    n_sp, rows_ref, cot_ref, stats_ref, full_rows, full_cot, all_stats,
    local_sem, stat_send, stat_recv, sp_send, sp_recv, tp_send, tp_recv,
):
    n_tp = 4
    sp, tp = lax.axis_index("sp"), lax.axis_index("tp")
    width = rows_ref.shape[2]
    arrays = ((rows_ref, full_rows), (cot_ref, full_cot))
    greet(sp, tp, n_sp, n_tp)
    started = []

    def from_sp(which, step):
        source, target = arrays[which]
        peer = flip(sp, step)
        return pltpu.make_async_remote_copy(
            src_ref=source.at[peer],
            dst_ref=target.at[sp, :, columns(tp, width)],
            send_sem=sp_send.at[which, step],
            recv_sem=sp_recv.at[which, step],
            device_id=(peer, tp),
            device_id_type=MESH,
        )

    def along_tp(which, step, origin, hop, slot):
        target = arrays[which][1]
        block = target.at[flip(sp, step), :, columns(flip(tp, origin), width)]
        return pltpu.make_async_remote_copy(
            src_ref=block,
            dst_ref=block,
            send_sem=tp_send.at[which, step, slot],
            recv_sem=tp_recv.at[which, step, slot],
            device_id=(sp, flip(tp, hop)),
            device_id_type=MESH,
        )

    own = []
    for which in range(2):
        source, target = arrays[which]
        copy = pltpu.make_async_copy(
            source.at[sp], target.at[sp, :, columns(tp, width)], local_sem.at[which]
        )
        copy.start()
        own.append(copy)
        for step in range(1, n_sp):
            copy = from_sp(which, step)
            copy.start()
            started.append(copy)
    stat_copies = []
    for mask in range(1, n_tp):
        copy = pltpu.make_async_remote_copy(
            src_ref=stats_ref,
            dst_ref=all_stats.at[mask],
            send_sem=stat_send.at[mask],
            recv_sem=stat_recv.at[mask],
            device_id=(sp, flip(tp, mask)),
            device_id_type=MESH,
        )
        copy.start()
        stat_copies.append(copy)
    all_stats[0] = stats_ref[...]

    lag = 1
    work = [(which, step) for which in range(2) for step in range(n_sp)]
    hops = {}
    for turn in range(len(work) + lag):
        if turn < len(work):
            which, step = work[turn]
            if step == 0:
                own[which].wait()
            else:
                from_sp(which, step).wait_recv()
            first, second = (1, 2) if step % 2 == 0 else (2, 1)
            near = along_tp(which, step, 0, first, 0)
            near.start()
            far = along_tp(which, step, 0, second, 1)
            far.start()
            hops[turn] = (near, far)
        if turn >= lag:
            which, step = work[turn - lag]
            first, second = (1, 2) if step % 2 == 0 else (2, 1)
            near, far = hops[turn - lag]
            near.wait_recv()
            onward = along_tp(which, step, first, second, 2)
            onward.start()
            hops[turn - lag] = (near, far, onward)
    for turn in range(len(work)):
        near, far, onward = hops[turn]
        far.wait_recv()
        onward.wait_recv()
        near.wait_send()
        far.wait_send()
        onward.wait_send()
    for copy in started:
        copy.wait_send()
    for copy in stat_copies:
        copy.wait()


def dispatch(sent_rows, sent_cot, stats, n_sp):
    experts, capacity, width = sent_rows.shape
    full = jax.ShapeDtypeStruct((experts, capacity, 4 * width), sent_rows.dtype)
    vmem = pl.BlockSpec(memory_space=pltpu.VMEM)
    dma = pltpu.SemaphoreType.DMA
    return pl.pallas_call(
        functools.partial(dispatch_kernel, n_sp),
        out_shape=(full, full, jax.ShapeDtypeStruct((4,) + stats.shape, stats.dtype)),
        in_specs=[vmem] * 3,
        out_specs=(vmem,) * 3,
        scratch_shapes=[
            dma((2,)), dma((4,)), dma((4,)),
            dma((2, n_sp)), dma((2, n_sp)), dma((2, n_sp, 3)), dma((2, n_sp, 3)),
        ],
        compiler_params=pltpu.CompilerParams(collective_id=0, has_side_effects=True),
    )(sent_rows, sent_cot, stats)


def return_kernel(
    n_sp, partial_ref, out_ref, landed, passing, finished, tp_send, tp_recv, sp_send, sp_recv
):
    n_tp = 4
    sp, tp = lax.axis_index("sp"), lax.axis_index("tp")
    width = out_ref.shape[2]
    greet(sp, tp, n_sp, n_tp)

    def order(turn):
        return (1, 2) if turn % 2 == 0 else (2, 1)

    def step_of(turn):
        return n_sp - 1 - turn

    def piece(turn, mask):
        return partial_ref.at[flip(sp, step_of(turn)), :, columns(flip(tp, mask), width)]

    def along_tp(turn, source, hop, slot):
        return pltpu.make_async_remote_copy(
            src_ref=source,
            dst_ref=landed.at[turn, slot],
            send_sem=tp_send.at[turn, slot],
            recv_sem=tp_recv.at[turn, slot],
            device_id=(sp, flip(tp, hop)),
            device_id_type=MESH,
        )

    def read(turn, mask):
        return piece(turn, mask)[...].astype(jnp.float32)

    crossing, direct, summed, home = {}, {}, {}, {}
    for turn in range(n_sp):
        first, second = order(turn)
        crossing[turn] = along_tp(turn, piece(turn, first + second), first, 1)
        crossing[turn].start()
        direct[turn] = along_tp(turn, piece(turn, first), first, 0)
        direct[turn].start()
    for turn in range(n_sp + 1):
        if turn < n_sp:
            first, second = order(turn)
            crossing[turn].wait_recv()
            passing[turn] = (
                read(turn, second) + landed[turn, 1].astype(jnp.float32)
            ).astype(passing.dtype)
            summed[turn] = along_tp(turn, passing.at[turn], second, 2)
            summed[turn].start()
        if turn >= 1:
            last = turn - 1
            direct[last].wait_recv()
            summed[last].wait_recv()
            total = (
                read(last, 0)
                + landed[last, 0].astype(jnp.float32)
                + landed[last, 2].astype(jnp.float32)
            ).astype(finished.dtype)
            step = step_of(last)
            if step == 0:
                out_ref[sp] = total
            else:
                finished[step] = total
                home[step] = pltpu.make_async_remote_copy(
                    src_ref=finished.at[step],
                    dst_ref=out_ref.at[sp],
                    send_sem=sp_send.at[step],
                    recv_sem=sp_recv.at[step],
                    device_id=(flip(sp, step), tp),
                    device_id_type=MESH,
                )
                home[step].start()
    for turn in range(n_sp):
        crossing[turn].wait_send()
        direct[turn].wait_send()
        summed[turn].wait_send()
    for step in range(1, n_sp):
        home[step].wait()


def send_home(partial, n_sp):
    experts, capacity, full = partial.shape
    width = full // 4
    vmem = pl.BlockSpec(memory_space=pltpu.VMEM)
    dma = pltpu.SemaphoreType.DMA
    return pl.pallas_call(
        functools.partial(return_kernel, n_sp),
        out_shape=jax.ShapeDtypeStruct((experts, capacity, width), partial.dtype),
        in_specs=[vmem],
        out_specs=vmem,
        scratch_shapes=[
            pltpu.VMEM((n_sp, 3, capacity, width), partial.dtype),
            pltpu.VMEM((n_sp, capacity, width), partial.dtype),
            pltpu.VMEM((n_sp, capacity, width), partial.dtype),
            dma((n_sp, 3)), dma((n_sp, 3)), dma((n_sp,)), dma((n_sp,)),
        ],
        compiler_params=pltpu.CompilerParams(collective_id=1, has_side_effects=True),
    )(partial)


def contract_rows(left, right):
    return lax.dot_general(
        left, right, (((0,), (0,)), ((), ())), preferred_element_type=jnp.float32
    )


def contract_cols(left, right):
    return lax.dot_general(
        left, right, (((1,), (1,)), ((), ())), preferred_element_type=jnp.float32
    )


def expert_backward(token_rows, cot_rows, gate_matrix, up_matrix, down_matrix):
    gate_pre = contract_cols(token_rows, gate_matrix)
    up_pre = contract_cols(token_rows, up_matrix)
    gate_sigmoid = jax.nn.sigmoid(gate_pre)
    activation = gate_pre * gate_sigmoid
    hidden = (activation * up_pre).astype(jnp.bfloat16)
    grad_down = contract_rows(hidden, cot_rows)
    hidden_cot = contract_cols(cot_rows, down_matrix)
    up_cot = (hidden_cot * activation).astype(jnp.bfloat16)
    gate_cot = (
        hidden_cot * up_pre * gate_sigmoid * (1.0 + gate_pre * (1.0 - gate_sigmoid))
    ).astype(jnp.bfloat16)
    grad_gate = contract_rows(gate_cot, token_rows)
    grad_up = contract_rows(up_cot, token_rows)
    partial_value = jnp.dot(gate_cot, gate_matrix, preferred_element_type=jnp.float32) + jnp.dot(
        up_cot, up_matrix, preferred_element_type=jnp.float32
    )
    return (
        grad_gate[None],
        grad_up[None],
        grad_down[None],
        partial_value.astype(jnp.bfloat16)[None],
    )


def body(
    moe_input,
    out_cotangent,
    routes,
    route_weight,
    gate_weight,
    up_weight,
    down_weight,
    glu_value,
    glu_gate,
    conv_result,
    conv_taps,
    norm_gain,
    proj_weight,
):
    sp_count = lax.axis_size("sp")
    token_count = moe_input.shape[0]
    experts = sp_count * gate_weight.shape[0]
    capacity = 3 * token_count // experts
    target = pair_places(routes, experts, capacity).reshape(token_count, 2)
    slots = jnp.arange(experts * capacity, dtype=jnp.int32)[:, None]
    first_here, second_here = slots == target[None, :, 0], slots == target[None, :, 1]
    pick = (first_here | second_here).astype(jnp.bfloat16)
    slot_weight = jnp.sum(
        jnp.where(first_here, route_weight[None, :, 0], 0.0)
        + jnp.where(second_here, route_weight[None, :, 1], 0.0),
        axis=1,
    )
    shape = (experts, capacity, moe_input.shape[1])
    sent_rows = (
        jnp.dot(pick, moe_input, preferred_element_type=jnp.float32)
        .astype(jnp.bfloat16)
        .reshape(shape)
    )
    sent_cot = (
        (slot_weight[:, None] * jnp.dot(pick, out_cotangent, preferred_element_type=jnp.float32))
        .astype(jnp.bfloat16)
        .reshape(shape)
    )
    conv_values = conv_result.astype(jnp.float32)
    local_moments = jnp.stack(
        (jnp.sum(conv_values, axis=1), jnp.sum(conv_values * conv_values, axis=1))
    )
    own_kernels = lax.axis_size("tp") == 4 and gate_weight.shape[0] == 1
    if own_kernels:
        full_rows, full_cot, all_moments = dispatch(sent_rows, sent_cot, local_moments, sp_count)
        full_rows = full_rows.reshape(1, experts * capacity, -1)
        full_cot = full_cot.reshape(1, experts * capacity, -1)
        moments = jnp.sum(all_moments, axis=0)
    else:
        got_rows, got_cot = (
            lax.all_to_all(sent_rows, "sp", split_axis=0, concat_axis=1, tiled=True),
            lax.all_to_all(sent_cot, "sp", split_axis=0, concat_axis=1, tiled=True),
        )
        full_rows, full_cot = (
            lax.all_gather(got_rows, "tp", axis=2, tiled=True),
            lax.all_gather(got_cot, "tp", axis=2, tiled=True),
        )
        moments = lax.psum(local_moments, "tp")
    grad_gate, grad_up, grad_down, partial_value = expert_backward(
        full_rows[0], full_cot[0], gate_weight[0], up_weight[0], down_weight[0]
    )
    if own_kernels:
        returned = send_home(partial_value.reshape(experts, capacity, -1), sp_count)
    else:
        summed = lax.psum_scatter(partial_value, "tp", scatter_dimension=2, tiled=True)
        returned = lax.all_to_all(summed, "sp", split_axis=1, concat_axis=0, tiled=True)
    moe_grad = contract_rows(pick, returned.reshape(experts * capacity, -1))
    total_cot = (out_cotangent.astype(jnp.float32) + moe_grad).astype(jnp.bfloat16)
    row_mean = moments[0][:, None] / C
    row_var = moments[1][:, None] / C - row_mean * row_mean
    inv_scale = lax.rsqrt(row_var + NORM_EPS)
    normed = (conv_values - row_mean) * inv_scale
    linear = normed * norm_gain[None, :]
    lin_sigmoid = jax.nn.sigmoid(linear)
    act_out = (linear * lin_sigmoid).astype(jnp.bfloat16)
    cot_full = lax.all_gather(total_cot, "tp", axis=1, tiled=True)
    act_cot = contract_cols(cot_full, proj_weight)
    grad_proj = lax.psum_scatter(
        contract_rows(cot_full, act_out).astype(jnp.bfloat16), "sp", scatter_dimension=0, tiled=True
    ).astype(jnp.float32)
    norm_cot = act_cot * lin_sigmoid * (1.0 + linear * (1.0 - lin_sigmoid)) * norm_gain[None, :]
    cot_sums = lax.psum((jnp.sum(norm_cot, axis=1), jnp.sum(norm_cot * normed, axis=1)), "tp")
    conv_cot = inv_scale * (
        norm_cot - cot_sums[0][:, None] / C - normed * (cot_sums[1][:, None] / C)
    )
    reach_rows = conv_taps.shape[0] - 1
    next_block = from_behind(conv_cot[:reach_rows], "sp", -1)
    extended = jnp.concatenate([conv_cot, next_block], axis=0)
    glu_cot = lax.conv_general_dilated(
        extended[None],
        jnp.flip(conv_taps, 0)[:, None, :],
        (1,),
        "VALID",
        dimension_numbers=("NWC", "WIO", "NWC"),
        feature_group_count=conv_taps.shape[1],
        precision=lax.Precision.HIGHEST,
    )[0]
    gate_sigmoid = jax.nn.sigmoid(glu_gate.astype(jnp.float32))
    grad_value = (glu_cot * gate_sigmoid).astype(jnp.bfloat16)
    grad_glu_gate = (
        glu_cot * glu_value.astype(jnp.float32) * gate_sigmoid * (1.0 - gate_sigmoid)
    ).astype(jnp.bfloat16)
    return (grad_gate, grad_up, grad_down, grad_proj, grad_value, grad_glu_gate)


def solution(mesh):
    in_specs = (
        P("sp", "tp"),
        P("sp", "tp"),
        P("sp", None),
        P("sp", None),
        P("sp", "tp", None),
        P("sp", "tp", None),
        P("sp", "tp", None),
        P("sp", "tp"),
        P("sp", "tp"),
        P("sp", "tp"),
        P(None, "tp"),
        P("tp"),
        P("tp", None),
    )
    out_specs = (
        P("sp", "tp", None),
        P("sp", "tp", None),
        P("sp", "tp", None),
        P("sp", "tp"),
        P("sp", "tp"),
        P("sp", "tp"),
    )
    return jax.shard_map(body, mesh=mesh, in_specs=in_specs, out_specs=out_specs, check_vma=False)
```

```python
import functools

import jax
import jax.numpy as jnp
from jax import lax
from jax.experimental import pallas as pl
from jax.experimental.pallas import tpu as pltpu
from jax.sharding import PartitionSpec as P

C = 1024


NORM_EPS = 0.25


MESH = pl.DeviceIdType.MESH


def from_behind(value, axis, steps):
    count = lax.axis_size(axis)
    leading, last = (max(0, -steps), min(count, count - steps))
    return lax.ppermute(value, axis, [(source, source + steps) for source in range(leading, last)])


def pair_places(route_ids, experts, capacity):
    flat_ids = route_ids.reshape(-1)
    onehot = (flat_ids[:, None] == jnp.arange(experts, dtype=jnp.int32)[None, :]).astype(jnp.int32)
    earlier = jnp.cumsum(onehot, axis=0) - onehot
    slot_rank = jnp.sum(earlier * onehot, axis=1)
    return flat_ids * capacity + slot_rank


def place_rows(values, target, experts, capacity):
    empty_rows = jnp.zeros((experts * capacity, values.shape[1]), values.dtype)
    return empty_rows.at[target].set(values).reshape(experts, capacity, values.shape[1])


def flip(index, mask):
    result, bit = index, 1
    while bit <= mask:
        if mask & bit:
            result = result + bit * (1 - 2 * ((index // bit) % 2))
        bit *= 2
    return result


def greet(sp, tp, n_sp, n_tp):
    barrier = pltpu.get_barrier_semaphore()
    for mask in range(1, n_sp):
        pl.semaphore_signal(barrier, inc=1, device_id=(flip(sp, mask), tp), device_id_type=MESH)
    for mask in range(1, n_tp):
        pl.semaphore_signal(barrier, inc=1, device_id=(sp, flip(tp, mask)), device_id_type=MESH)
    pl.semaphore_wait(barrier, n_sp + n_tp - 2)


def columns(index, width):
    return pl.ds(pl.multiple_of(index * width, width), width)


def dispatch_kernel(
    n_sp, rows_ref, cot_ref, stats_ref, full_rows, full_cot, all_stats,
    local_sem, stat_send, stat_recv, sp_send, sp_recv, tp_send, tp_recv,
):
    n_tp = 4
    sp, tp = lax.axis_index("sp"), lax.axis_index("tp")
    width = rows_ref.shape[2]
    arrays = ((rows_ref, full_rows), (cot_ref, full_cot))
    greet(sp, tp, n_sp, n_tp)
    started = []

    def from_sp(which, step):
        source, target = arrays[which]
        peer = flip(sp, step)
        return pltpu.make_async_remote_copy(
            src_ref=source.at[peer],
            dst_ref=target.at[sp, :, columns(tp, width)],
            send_sem=sp_send.at[which, step],
            recv_sem=sp_recv.at[which, step],
            device_id=(peer, tp),
            device_id_type=MESH,
        )

    def along_tp(which, step, origin, hop, slot):
        target = arrays[which][1]
        block = target.at[flip(sp, step), :, columns(flip(tp, origin), width)]
        return pltpu.make_async_remote_copy(
            src_ref=block,
            dst_ref=block,
            send_sem=tp_send.at[which, step, slot],
            recv_sem=tp_recv.at[which, step, slot],
            device_id=(sp, flip(tp, hop)),
            device_id_type=MESH,
        )

    own = []
    for which in range(2):
        source, target = arrays[which]
        copy = pltpu.make_async_copy(
            source.at[sp], target.at[sp, :, columns(tp, width)], local_sem.at[which]
        )
        copy.start()
        own.append(copy)
        for step in range(1, n_sp):
            copy = from_sp(which, step)
            copy.start()
            started.append(copy)
    stat_copies = []
    for mask in range(1, n_tp):
        copy = pltpu.make_async_remote_copy(
            src_ref=stats_ref,
            dst_ref=all_stats.at[mask],
            send_sem=stat_send.at[mask],
            recv_sem=stat_recv.at[mask],
            device_id=(sp, flip(tp, mask)),
            device_id_type=MESH,
        )
        copy.start()
        stat_copies.append(copy)
    all_stats[0] = stats_ref[...]

    lag = 2
    work = [(which, step) for which in range(2) for step in range(n_sp)]
    hops = {}
    for turn in range(len(work) + lag):
        if turn < len(work):
            which, step = work[turn]
            if step == 0:
                own[which].wait()
            else:
                from_sp(which, step).wait_recv()
            first, second = (1, 2) if step % 2 == 0 else (2, 1)
            near = along_tp(which, step, 0, first, 0)
            near.start()
            far = along_tp(which, step, 0, second, 1)
            far.start()
            hops[turn] = (near, far)
        if turn >= lag:
            which, step = work[turn - lag]
            first, second = (1, 2) if step % 2 == 0 else (2, 1)
            near, far = hops[turn - lag]
            near.wait_recv()
            onward = along_tp(which, step, first, second, 2)
            onward.start()
            hops[turn - lag] = (near, far, onward)
    for turn in range(len(work)):
        near, far, onward = hops[turn]
        far.wait_recv()
        onward.wait_recv()
        near.wait_send()
        far.wait_send()
        onward.wait_send()
    for copy in started:
        copy.wait_send()
    for copy in stat_copies:
        copy.wait()


def dispatch(sent_rows, sent_cot, stats, n_sp):
    experts, capacity, width = sent_rows.shape
    full = jax.ShapeDtypeStruct((experts, capacity, 4 * width), sent_rows.dtype)
    vmem = pl.BlockSpec(memory_space=pltpu.VMEM)
    dma = pltpu.SemaphoreType.DMA
    return pl.pallas_call(
        functools.partial(dispatch_kernel, n_sp),
        out_shape=(full, full, jax.ShapeDtypeStruct((4,) + stats.shape, stats.dtype)),
        in_specs=[vmem] * 3,
        out_specs=(vmem,) * 3,
        scratch_shapes=[
            dma((2,)), dma((4,)), dma((4,)),
            dma((2, n_sp)), dma((2, n_sp)), dma((2, n_sp, 3)), dma((2, n_sp, 3)),
        ],
        compiler_params=pltpu.CompilerParams(collective_id=0, has_side_effects=True),
    )(sent_rows, sent_cot, stats)


def return_kernel(
    n_sp, partial_ref, out_ref, landed, passing, finished, tp_send, tp_recv, sp_send, sp_recv
):
    n_tp = 4
    sp, tp = lax.axis_index("sp"), lax.axis_index("tp")
    width = out_ref.shape[2]
    greet(sp, tp, n_sp, n_tp)

    def order(turn):
        return (1, 2) if turn % 2 == 0 else (2, 1)

    def step_of(turn):
        return n_sp - 1 - turn

    def piece(turn, mask):
        return partial_ref.at[flip(sp, step_of(turn)), :, columns(flip(tp, mask), width)]

    def along_tp(turn, source, hop, slot):
        return pltpu.make_async_remote_copy(
            src_ref=source,
            dst_ref=landed.at[turn, slot],
            send_sem=tp_send.at[turn, slot],
            recv_sem=tp_recv.at[turn, slot],
            device_id=(sp, flip(tp, hop)),
            device_id_type=MESH,
        )

    def read(turn, mask):
        return piece(turn, mask)[...].astype(jnp.float32)

    crossing, direct, summed, home = {}, {}, {}, {}

    def send_out(turn):
        first, second = order(turn)
        crossing[turn] = along_tp(turn, piece(turn, first + second), first, 1)
        crossing[turn].start()
        direct[turn] = along_tp(turn, piece(turn, first), first, 0)
        direct[turn].start()

    ahead = min(2, n_sp)
    for turn in range(ahead):
        send_out(turn)
    for turn in range(n_sp + 1):
        if turn < n_sp:
            first, second = order(turn)
            crossing[turn].wait_recv()
            passing[turn] = (
                read(turn, second) + landed[turn, 1].astype(jnp.float32)
            ).astype(passing.dtype)
            summed[turn] = along_tp(turn, passing.at[turn], second, 2)
            summed[turn].start()
            if turn + ahead < n_sp:
                send_out(turn + ahead)
        if turn >= 1:
            last = turn - 1
            direct[last].wait_recv()
            summed[last].wait_recv()
            total = (
                read(last, 0)
                + landed[last, 0].astype(jnp.float32)
                + landed[last, 2].astype(jnp.float32)
            ).astype(finished.dtype)
            step = step_of(last)
            if step == 0:
                out_ref[sp] = total
            else:
                finished[step] = total
                home[step] = pltpu.make_async_remote_copy(
                    src_ref=finished.at[step],
                    dst_ref=out_ref.at[sp],
                    send_sem=sp_send.at[step],
                    recv_sem=sp_recv.at[step],
                    device_id=(flip(sp, step), tp),
                    device_id_type=MESH,
                )
                home[step].start()
    for turn in range(n_sp):
        crossing[turn].wait_send()
        direct[turn].wait_send()
        summed[turn].wait_send()
    for step in range(1, n_sp):
        home[step].wait()


def send_home(partial, n_sp):
    experts, capacity, full = partial.shape
    width = full // 4
    vmem = pl.BlockSpec(memory_space=pltpu.VMEM)
    dma = pltpu.SemaphoreType.DMA
    return pl.pallas_call(
        functools.partial(return_kernel, n_sp),
        out_shape=jax.ShapeDtypeStruct((experts, capacity, width), partial.dtype),
        in_specs=[vmem],
        out_specs=vmem,
        scratch_shapes=[
            pltpu.VMEM((n_sp, 3, capacity, width), partial.dtype),
            pltpu.VMEM((n_sp, capacity, width), partial.dtype),
            pltpu.VMEM((n_sp, capacity, width), partial.dtype),
            dma((n_sp, 3)), dma((n_sp, 3)), dma((n_sp,)), dma((n_sp,)),
        ],
        compiler_params=pltpu.CompilerParams(collective_id=1, has_side_effects=True),
    )(partial)


def gather_kernel(block_ref, full_ref, local_sem, send_sem, recv_sem):
    sp, tp = lax.axis_index("sp"), lax.axis_index("tp")
    chunks, _, width = block_ref.shape
    barrier = pltpu.get_barrier_semaphore()
    for mask in (1, 2):
        pl.semaphore_signal(barrier, inc=1, device_id=(sp, flip(tp, mask)), device_id_type=MESH)
    pl.semaphore_wait(barrier, 2)

    def along_tp(chunk, source, origin, hop, slot):
        return pltpu.make_async_remote_copy(
            src_ref=source,
            dst_ref=full_ref.at[chunk, :, columns(flip(tp, origin), width)],
            send_sem=send_sem.at[chunk, slot],
            recv_sem=recv_sem.at[chunk, slot],
            device_id=(sp, flip(tp, hop)),
            device_id_type=MESH,
        )

    hops = []
    for chunk in range(chunks):
        first, second = (1, 2) if chunk % 2 == 0 else (2, 1)
        near = along_tp(chunk, block_ref.at[chunk], 0, first, 0)
        near.start()
        hops.append([near])
    own = pltpu.make_async_copy(block_ref, full_ref.at[:, :, columns(tp, width)], local_sem)
    own.start()
    for chunk in range(chunks):
        first, second = (1, 2) if chunk % 2 == 0 else (2, 1)
        far = along_tp(chunk, block_ref.at[chunk], 0, second, 1)
        far.start()
        hops[chunk].append(far)
    for chunk in range(chunks):
        first, second = (1, 2) if chunk % 2 == 0 else (2, 1)
        hops[chunk][0].wait_recv()
        source = full_ref.at[chunk, :, columns(flip(tp, first), width)]
        onward = along_tp(chunk, source, first, second, 2)
        onward.start()
        hops[chunk].append(onward)
    own.wait()
    for near, far, onward in hops:
        near.wait_send()
        far.wait()
        onward.wait()


def gather_features(block, chunks):
    rows, width = block.shape
    vmem = pl.BlockSpec(memory_space=pltpu.VMEM)
    dma = pltpu.SemaphoreType.DMA
    full = pl.pallas_call(
        gather_kernel,
        out_shape=jax.ShapeDtypeStruct((chunks, rows // chunks, 4 * width), block.dtype),
        in_specs=[vmem],
        out_specs=vmem,
        scratch_shapes=[dma(()), dma((chunks, 3)), dma((chunks, 3))],
        compiler_params=pltpu.CompilerParams(collective_id=2, has_side_effects=True),
    )(block.reshape(chunks, rows // chunks, width))
    return full.reshape(rows, -1)


def contract_rows(left, right):
    return lax.dot_general(
        left, right, (((0,), (0,)), ((), ())), preferred_element_type=jnp.float32
    )


def contract_cols(left, right):
    return lax.dot_general(
        left, right, (((1,), (1,)), ((), ())), preferred_element_type=jnp.float32
    )


def expert_backward(token_rows, cot_rows, gate_matrix, up_matrix, down_matrix):
    gate_pre = contract_cols(token_rows, gate_matrix)
    up_pre = contract_cols(token_rows, up_matrix)
    gate_sigmoid = jax.nn.sigmoid(gate_pre)
    activation = gate_pre * gate_sigmoid
    hidden = (activation * up_pre).astype(jnp.bfloat16)
    grad_down = contract_rows(hidden, cot_rows)
    hidden_cot = contract_cols(cot_rows, down_matrix)
    up_cot = (hidden_cot * activation).astype(jnp.bfloat16)
    gate_cot = (
        hidden_cot * up_pre * gate_sigmoid * (1.0 + gate_pre * (1.0 - gate_sigmoid))
    ).astype(jnp.bfloat16)
    grad_gate = contract_rows(gate_cot, token_rows)
    grad_up = contract_rows(up_cot, token_rows)
    partial_value = jnp.dot(gate_cot, gate_matrix, preferred_element_type=jnp.float32) + jnp.dot(
        up_cot, up_matrix, preferred_element_type=jnp.float32
    )
    return (
        grad_gate[None],
        grad_up[None],
        grad_down[None],
        partial_value.astype(jnp.bfloat16)[None],
    )


def body(
    moe_input,
    out_cotangent,
    routes,
    route_weight,
    gate_weight,
    up_weight,
    down_weight,
    glu_value,
    glu_gate,
    conv_result,
    conv_taps,
    norm_gain,
    proj_weight,
):
    sp_count = lax.axis_size("sp")
    token_count = moe_input.shape[0]
    experts = sp_count * gate_weight.shape[0]
    capacity = 3 * token_count // experts
    target = pair_places(routes, experts, capacity).reshape(token_count, 2)
    slots = jnp.arange(experts * capacity, dtype=jnp.int32)[:, None]
    first_here, second_here = slots == target[None, :, 0], slots == target[None, :, 1]
    pick = (first_here | second_here).astype(jnp.bfloat16)
    slot_weight = jnp.sum(
        jnp.where(first_here, route_weight[None, :, 0], 0.0)
        + jnp.where(second_here, route_weight[None, :, 1], 0.0),
        axis=1,
    )
    shape = (experts, capacity, moe_input.shape[1])
    sent_rows = (
        jnp.dot(pick, moe_input, preferred_element_type=jnp.float32)
        .astype(jnp.bfloat16)
        .reshape(shape)
    )
    sent_cot = (
        (slot_weight[:, None] * jnp.dot(pick, out_cotangent, preferred_element_type=jnp.float32))
        .astype(jnp.bfloat16)
        .reshape(shape)
    )
    conv_values = conv_result.astype(jnp.float32)
    local_moments = jnp.stack(
        (jnp.sum(conv_values, axis=1), jnp.sum(conv_values * conv_values, axis=1))
    )
    own_kernels = lax.axis_size("tp") == 4 and gate_weight.shape[0] == 1
    if own_kernels:
        full_rows, full_cot, all_moments = dispatch(sent_rows, sent_cot, local_moments, sp_count)
        full_rows = full_rows.reshape(1, experts * capacity, -1)
        full_cot = full_cot.reshape(1, experts * capacity, -1)
        moments = jnp.sum(all_moments, axis=0)
    else:
        got_rows, got_cot = (
            lax.all_to_all(sent_rows, "sp", split_axis=0, concat_axis=1, tiled=True),
            lax.all_to_all(sent_cot, "sp", split_axis=0, concat_axis=1, tiled=True),
        )
        full_rows, full_cot = (
            lax.all_gather(got_rows, "tp", axis=2, tiled=True),
            lax.all_gather(got_cot, "tp", axis=2, tiled=True),
        )
        moments = lax.psum(local_moments, "tp")
    grad_gate, grad_up, grad_down, partial_value = expert_backward(
        full_rows[0], full_cot[0], gate_weight[0], up_weight[0], down_weight[0]
    )
    if own_kernels:
        returned = send_home(partial_value.reshape(experts, capacity, -1), sp_count)
    else:
        summed = lax.psum_scatter(partial_value, "tp", scatter_dimension=2, tiled=True)
        returned = lax.all_to_all(summed, "sp", split_axis=1, concat_axis=0, tiled=True)
    moe_grad = contract_rows(pick, returned.reshape(experts * capacity, -1))
    total_cot = (out_cotangent.astype(jnp.float32) + moe_grad).astype(jnp.bfloat16)
    row_mean = moments[0][:, None] / C
    row_var = moments[1][:, None] / C - row_mean * row_mean
    inv_scale = lax.rsqrt(row_var + NORM_EPS)
    normed = (conv_values - row_mean) * inv_scale
    linear = normed * norm_gain[None, :]
    lin_sigmoid = jax.nn.sigmoid(linear)
    act_out = (linear * lin_sigmoid).astype(jnp.bfloat16)
    if own_kernels:
        cot_full = gather_features(total_cot, 4 if token_count % 32 == 0 else 1)
    else:
        cot_full = lax.all_gather(total_cot, "tp", axis=1, tiled=True)
    act_cot = contract_cols(cot_full, proj_weight)
    grad_proj = lax.psum_scatter(
        contract_rows(cot_full, act_out).astype(jnp.bfloat16), "sp", scatter_dimension=0, tiled=True
    ).astype(jnp.float32)
    norm_cot = act_cot * lin_sigmoid * (1.0 + linear * (1.0 - lin_sigmoid)) * norm_gain[None, :]
    cot_sums = lax.psum((jnp.sum(norm_cot, axis=1), jnp.sum(norm_cot * normed, axis=1)), "tp")
    conv_cot = inv_scale * (
        norm_cot - cot_sums[0][:, None] / C - normed * (cot_sums[1][:, None] / C)
    )
    reach_rows = conv_taps.shape[0] - 1
    next_block = from_behind(conv_cot[:reach_rows], "sp", -1)
    extended = jnp.concatenate([conv_cot, next_block], axis=0)
    glu_cot = lax.conv_general_dilated(
        extended[None],
        jnp.flip(conv_taps, 0)[:, None, :],
        (1,),
        "VALID",
        dimension_numbers=("NWC", "WIO", "NWC"),
        feature_group_count=conv_taps.shape[1],
        precision=lax.Precision.HIGHEST,
    )[0]
    gate_sigmoid = jax.nn.sigmoid(glu_gate.astype(jnp.float32))
    grad_value = (glu_cot * gate_sigmoid).astype(jnp.bfloat16)
    grad_glu_gate = (
        glu_cot * glu_value.astype(jnp.float32) * gate_sigmoid * (1.0 - gate_sigmoid)
    ).astype(jnp.bfloat16)
    return (grad_gate, grad_up, grad_down, grad_proj, grad_value, grad_glu_gate)


def solution(mesh):
    in_specs = (
        P("sp", "tp"),
        P("sp", "tp"),
        P("sp", None),
        P("sp", None),
        P("sp", "tp", None),
        P("sp", "tp", None),
        P("sp", "tp", None),
        P("sp", "tp"),
        P("sp", "tp"),
        P("sp", "tp"),
        P(None, "tp"),
        P("tp"),
        P("tp", None),
    )
    out_specs = (
        P("sp", "tp", None),
        P("sp", "tp", None),
        P("sp", "tp", None),
        P("sp", "tp"),
        P("sp", "tp"),
        P("sp", "tp"),
    )
    return jax.shard_map(body, mesh=mesh, in_specs=in_specs, out_specs=out_specs, check_vma=False)
```
